32 devices in a mesh: sp: 8 (over z, y), tp: 4 (over x, core).
Axes of the slice: x: 2, y: 2, z: 4, core: 2. Of those that a mesh axis runs over, the one named last changes fastest.
Arguments:
- tokens: bfloat16 [8192, 2048], P('sp', 'tp'), may hold values from -6 to 6
- mix_gain: float32 [2048], replicated, may hold values from 0.1 to 1.9
- query_weight: bfloat16 [2048, 1024], P('sp', 'tp'), may hold values from -0.125 to 0.125
- key_weight: bfloat16 [2048, 256], P('sp', 'tp'), may hold values from -0.125 to 0.125
- value_weight: bfloat16 [2048, 256], P('sp', 'tp'), may hold values from -0.125 to 0.125
- conv_value_weight: bfloat16 [2048, 1024], P('sp', 'tp'), may hold values from -0.125 to 0.125
- conv_gate_weight: bfloat16 [2048, 1024], P('sp', 'tp'), may hold values from -0.125 to 0.125
- query_gain: float32 [64], replicated, may hold values from 0.1 to 1.9
- key_gain: float32 [64], replicated, may hold values from 0.1 to 1.9
- sink_logit: float32 [16], P('tp'), may hold values from 3 to 7
- conv_taps: float32 [31, 1024], P(None, 'tp'), may hold values from -1 to 1
- conv_gain: float32 [1024], P('tp'), may hold values from 0.1 to 1.9
- attn_proj: bfloat16 [1024, 2048], P('tp', 'sp'), may hold values from -1.5 to 1.5
- conv_proj: bfloat16 [1024, 2048], P('tp', 'sp'), may hold values from -0.1875 to 0.1875
Outputs:
- mixed: bfloat16 [8192, 2048], P(('sp', 'tp'))
The draws below stay inside these ranges and needn't reach their ends.
All inputs are finite; a program needn't handle non-finite values.
Results may differ from the reference program's by a relative error of at most 0.0079.
Values may be sent and summed in bfloat16 or wider, within the bound.
No kernel may reach another device: no remote copies, remote signals or barrier semaphores. Data moves between devices by JAX's collectives and lax.ppermute only.
A program may use at most 128 MiB of HBM per device.

```python
import jax
import jax.numpy as jnp
from jax import lax

MODEL_DIM = 2048
QUERY_HEADS = 16
KEY_HEADS = 4
HEAD_DIM = 64
CHANNELS = 1024
KERNEL = 31
WINDOW = 128
LOCAL_TOKENS = 1024
TOKENS = 8192
CONV_REACH = 15


def levels(key, shape, shards, low, high):
    level = 1.0
    for dim, shards_of in shards:
        heights = jax.random.uniform(jax.random.fold_in(jax.random.fold_in(key, 6), dim), (shards_of,), jnp.float32, low / len(shards), high / len(shards))
        level = level * jnp.repeat(jnp.exp(heights), shape[dim] // shards_of).reshape((-1,) + (1,) * (len(shape) - 1 - dim))
    return level


def scatter_about(rng, shape, deviation, most, cuts=(), kind=jnp.bfloat16):
    drawn = jax.random.normal(rng, shape, jnp.float32) * deviation
    if len(cuts) > 0:
        drawn = levels(rng, shape, cuts, -0.22, 0.18) * drawn
    return jnp.clip(drawn, min=-most, max=most).astype(kind)


def setup_inputs(seed: int = 0) -> dict:
    seeds = jax.random.split(jax.random.key(seed), 15)
    return {
        "tokens": scatter_about(seeds[0], (TOKENS, MODEL_DIM), 1.0, 6.0, ((0, 8), (1, 4))),
        "mix_gain": jnp.clip(1.0 + 0.18 * jax.random.normal(seeds[1], (MODEL_DIM,), jnp.float32), 0.1, 1.9),
        "query_weight": scatter_about(seeds[2], (MODEL_DIM, QUERY_HEADS * HEAD_DIM), MODEL_DIM ** -0.5, 0.125, ((0, 8), (1, 4))),
        "key_weight": scatter_about(seeds[3], (MODEL_DIM, KEY_HEADS * HEAD_DIM), MODEL_DIM ** -0.5, 0.125, ((0, 8), (1, 4))),
        "value_weight": scatter_about(seeds[4], (MODEL_DIM, KEY_HEADS * HEAD_DIM), MODEL_DIM ** -0.5, 0.125, ((0, 8), (1, 4))),
        "conv_value_weight": scatter_about(seeds[5], (MODEL_DIM, CHANNELS), MODEL_DIM ** -0.5, 0.125, ((0, 8), (1, 4))),
        "conv_gate_weight": scatter_about(seeds[6], (MODEL_DIM, CHANNELS), MODEL_DIM ** -0.5, 0.125, ((0, 8), (1, 4))),
        "query_gain": jnp.clip(1.0 + 0.18 * jax.random.normal(seeds[7], (HEAD_DIM,), jnp.float32), 0.1, 1.9),
        "key_gain": jnp.clip(1.0 + 0.18 * jax.random.normal(seeds[8], (HEAD_DIM,), jnp.float32), 0.1, 1.9),
        "sink_logit": jnp.clip(3.0 + 4.0 * jax.random.uniform(seeds[9], (QUERY_HEADS,), jnp.float32) ** levels(seeds[9], (QUERY_HEADS,), ((0, 4),), -0.2, 0.2), 3.0, 7.0),
        "conv_taps": scatter_about(seeds[10], (KERNEL, CHANNELS), KERNEL ** -0.5, 1.0, ((1, 4),), jnp.float32),
        "conv_gain": jnp.clip(1.0 + 0.18 * jax.random.normal(seeds[11], (CHANNELS,), jnp.float32), 0.1, 1.9),
        "attn_proj": scatter_about(seeds[12], (QUERY_HEADS * HEAD_DIM, MODEL_DIM), (QUERY_HEADS * HEAD_DIM // 64) ** -0.5, 1.5, ((0, 4), (1, 8))),
        "conv_proj": scatter_about(seeds[13], (CHANNELS, MODEL_DIM), CHANNELS ** -0.5, 0.1875, ((0, 4), (1, 8))),
    }


EPSILON = 0.1

def unit_rows(values, gain):
    return values * lax.rsqrt(lax.optimization_barrier(jnp.mean(values * values, axis=-1, keepdims=True)) + EPSILON) * gain

def attend(queries, keys, values, sinks, offset, total):
    scale = queries.shape[-1] ** (-0.5)
    scores = jnp.einsum('qkgd,skd->kgqs', queries.astype(jnp.float32), keys.astype(jnp.float32)) * scale
    query_pos = offset + jnp.arange(queries.shape[0], dtype=jnp.int32)
    key_pos = offset - WINDOW + jnp.arange(keys.shape[0], dtype=jnp.int32)
    allowed = (jnp.abs(key_pos[None, :] - query_pos[:, None]) <= WINDOW) & (key_pos[None, :] >= 0) & (key_pos[None, :] < total)
    weights = jnp.where(allowed, jnp.exp(scores), 0.0)
    denominator = lax.optimization_barrier(jnp.sum(weights, axis=-1, keepdims=True)) + jnp.exp(sinks).reshape(keys.shape[1], -1, 1, 1)
    shares = (weights / denominator).astype(jnp.bfloat16)
    result = jnp.einsum('kgqs,skd->qkgd', shares.astype(jnp.float32), values.astype(jnp.float32))
    return result.reshape(queries.shape[0], -1).astype(jnp.bfloat16)

def depthwise(extended, kernel_taps, count):
    result = jnp.zeros((count, kernel_taps.shape[1]), jnp.float32)
    for offset in range(kernel_taps.shape[0]):
        result = result + kernel_taps[offset] * extended[offset:offset + count].astype(jnp.float32)
    return result

def reference(tokens, mix_gain, query_weight, key_weight, value_weight, conv_value_weight, conv_gate_weight, query_gain, key_gain, sink_logit, conv_taps, conv_gain, attn_proj, conv_proj):
    total = tokens.shape[0]
    normed = unit_rows(tokens.astype(jnp.float32), mix_gain).astype(jnp.bfloat16)
    query = jnp.dot(normed, query_weight, preferred_element_type=jnp.float32)
    key_part = jnp.dot(normed, key_weight, preferred_element_type=jnp.float32)
    value_part = jnp.dot(normed, value_weight, preferred_element_type=jnp.float32)
    conv_value = jnp.dot(normed, conv_value_weight, preferred_element_type=jnp.float32)
    conv_gate = jnp.dot(normed, conv_gate_weight, preferred_element_type=jnp.float32)
    group = QUERY_HEADS // KEY_HEADS
    queries = unit_rows(query.reshape(total, KEY_HEADS, group, HEAD_DIM), query_gain).astype(jnp.bfloat16)
    keys = unit_rows(key_part.reshape(total, KEY_HEADS, HEAD_DIM), key_gain).astype(jnp.bfloat16)
    values = value_part.reshape(total, KEY_HEADS, HEAD_DIM).astype(jnp.bfloat16)
    padded_keys = jnp.pad(keys, ((WINDOW, WINDOW), (0, 0), (0, 0)))
    padded_values = jnp.pad(values, ((WINDOW, WINDOW), (0, 0), (0, 0)))

    def one_block(index):
        begin = (index * LOCAL_TOKENS).astype(jnp.int32)
        block_queries = lax.dynamic_slice_in_dim(queries, begin, LOCAL_TOKENS, 0)
        block_keys = lax.dynamic_slice_in_dim(padded_keys, begin, LOCAL_TOKENS + 2 * WINDOW, 0)
        block_values = lax.dynamic_slice_in_dim(padded_values, begin, LOCAL_TOKENS + 2 * WINDOW, 0)
        return attend(block_queries, block_keys, block_values, sink_logit, begin, total)
    attended = lax.map(one_block, jnp.arange(total // LOCAL_TOKENS, dtype=jnp.int32)).reshape(total, -1)
    gated = (conv_value * jax.nn.sigmoid(conv_gate)).astype(jnp.bfloat16)
    extended = jnp.pad(gated, ((CONV_REACH, CONV_REACH), (0, 0)))
    convolved = depthwise(extended, conv_taps, total)
    center = lax.optimization_barrier(jnp.mean(convolved, axis=1, keepdims=True))
    centered = convolved - center
    spread = lax.optimization_barrier(jnp.mean(centered * centered, axis=1, keepdims=True))
    featured = jax.nn.silu(centered * lax.rsqrt(spread + EPSILON) * conv_gain).astype(jnp.bfloat16)
    summed = jnp.dot(attended, attn_proj, preferred_element_type=jnp.float32) + jnp.dot(featured, conv_proj, preferred_element_type=jnp.float32)
    return summed.astype(jnp.bfloat16)
```

```python
import jax
import jax.numpy as jnp
from jax import lax
from jax.experimental import pallas as pl
from jax.experimental.pallas import tpu as pltpu
from jax.sharding import PartitionSpec as P

WINDOW = 128
HALO = 16


EPSILON = 0.1


def unit_rows(values, gain):
    return values * lax.rsqrt(jnp.mean(values * values, axis=-1, keepdims=True) + EPSILON) * gain


def gather_line(value, axis):
    size = lax.axis_size(axis)
    pair = 2 if size % 2 == 0 else 1
    line = size // pair
    index = lax.axis_index(axis)
    spot = index // pair

    def across(piece, valid):
        pairs = [(i, i ^ 1) for i in range(size) if valid(i // pair)]
        return lax.ppermute(piece, axis, pairs)

    ups, downs = {}, {}
    up = down = value
    if pair == 2:
        other = across(value, lambda spot: True)
    cross_up, cross_down = {}, {}
    for k in range(1, line):
        up = lax.ppermute(
            up, axis, [(i, i + pair) for i in range(size - pair) if i // pair >= k - 1]
        )
        down = lax.ppermute(
            down, axis, [(i, i - pair) for i in range(pair, size) if i // pair + k - 1 < line]
        )
        ups[k], downs[k] = up, down
        if pair == 2:
            cross_up[k] = across(up, lambda spot, k=k: spot >= k)
            cross_down[k] = across(down, lambda spot, k=k: spot + k < line)
    out = jnp.zeros((size,) + value.shape, value.dtype)
    zeros = (0,) * value.ndim

    def put(out, piece, where):
        return lax.dynamic_update_slice(out, piece[None], (where,) + zeros)

    out = put(out, value, index)
    if pair == 2:
        out = put(out, other, index ^ 1)
    for k in range(1, line):
        place = ((spot - k) % line) * pair
        low = index % pair
        own = jnp.where(spot >= k, ups[k], downs[line - k])
        out = put(out, own, place + low)
        if pair == 2:
            crossed = jnp.where(spot >= k, cross_up[k], cross_down[line - k])
            out = put(out, crossed, place + (1 - low))
    return out


def gather_columns(tokens, axis):
    size = lax.axis_size(axis)
    if size != 4:
        return lax.all_gather(tokens, axis, axis=1, tiled=True)
    index = lax.axis_index(axis)
    far = lax.ppermute(tokens, axis, [(i, i ^ 2) for i in range(size)])
    near = [(i, i ^ 1) for i in range(size)]
    own_other = lax.ppermute(tokens, axis, near)
    far_other = lax.ppermute(far, axis, near)
    first = index < 2
    even = index % 2 == 0
    own_pair = (jnp.where(even, tokens, own_other), jnp.where(even, own_other, tokens))
    far_pair = (jnp.where(even, far, far_other), jnp.where(even, far_other, far))
    low = [jnp.where(first, a, b) for a, b in zip(own_pair, far_pair)]
    high = [jnp.where(first, b, a) for a, b in zip(own_pair, far_pair)]
    return jnp.concatenate(low + high, axis=1)


def scatter_sum(partial, axis):
    size = lax.axis_size(axis)
    if size != 4:
        return lax.psum_scatter(partial, axis, scatter_dimension=0, tiled=True)
    index = lax.axis_index(axis)
    x, core = index // 2, index % 2
    rows = partial.shape[0] // 4
    blocks = partial.reshape(2, 2, rows, partial.shape[1])
    kept = lax.dynamic_index_in_dim(blocks, core, 1, keepdims=False)
    sent = lax.dynamic_index_in_dim(blocks, 1 - core, 1, keepdims=False).astype(jnp.bfloat16)
    got = lax.ppermute(sent, axis, [(i, i ^ 1) for i in range(size)])
    away = lax.dynamic_index_in_dim(kept, 1 - x, 0, keepdims=False) + lax.dynamic_index_in_dim(
        got, 1 - x, 0, keepdims=False
    ).astype(jnp.float32)
    here = lax.dynamic_index_in_dim(kept, x, 0, keepdims=False) + lax.dynamic_index_in_dim(
        got, x, 0, keepdims=False
    ).astype(jnp.float32)
    came = lax.ppermute(away.astype(jnp.bfloat16), axis, [(i, i ^ 2) for i in range(size)])
    return here + came.astype(jnp.float32)


def attend(projected, kv, query_gain, sinks, offset, total, count, heads, local_kv):
    dim = query_gain.shape[0]
    group = heads // local_kv
    scale = dim ** (-0.5)
    span = 3 * WINDOW

    def kernel(place, sink, query, pairs, gain, out):
        start = pl.program_id(0) * WINDOW
        window = pairs[pl.ds(pl.multiple_of(start, WINDOW), span), :]
        row = lax.broadcasted_iota(jnp.int32, (WINDOW, span), 0)
        col = lax.broadcasted_iota(jnp.int32, (WINDOW, span), 1)
        key_pos = place[0] + start - WINDOW + col
        allowed = (
            (col >= row) & (col <= row + 2 * WINDOW) & (key_pos >= 0) & (key_pos < total)
        )
        results = []
        for head in range(heads):
            of = head // group
            keys = window[:, of * dim : (of + 1) * dim]
            values = window[:, (local_kv + of) * dim : (local_kv + of + 1) * dim]
            normed = unit_rows(query[:, head * dim : (head + 1) * dim], gain[...])
            scores = lax.dot_general(
                normed.astype(jnp.bfloat16),
                keys,
                (((1,), (1,)), ((), ())),
                preferred_element_type=jnp.float32,
            )
            weights = jnp.where(allowed, jnp.exp(scores * scale), 0.0)
            denominator = jnp.sum(weights, axis=-1, keepdims=True) + sink[head]
            shares = (weights * (1.0 / denominator)).astype(jnp.bfloat16)
            results.append(jnp.dot(shares, values, preferred_element_type=jnp.float32))
        out[...] = jnp.concatenate(results, axis=1).astype(jnp.bfloat16)

    width = heads * dim
    return pl.pallas_call(
        kernel,
        grid=(count // WINDOW,),
        in_specs=[
            pl.BlockSpec(memory_space=pltpu.SMEM),
            pl.BlockSpec(memory_space=pltpu.SMEM),
            pl.BlockSpec((WINDOW, width), lambda i: (i, 0)),
            pl.BlockSpec(kv.shape, lambda i: (0, 0)),
            pl.BlockSpec((1, dim), lambda i: (0, 0)),
        ],
        out_specs=pl.BlockSpec((WINDOW, width), lambda i: (i, 0)),
        out_shape=jax.ShapeDtypeStruct((count, width), jnp.bfloat16),
        name="attend",
    )(offset.reshape(1), jnp.exp(sinks), projected, kv, query_gain.reshape(1, dim))


def depthwise(extended, kernel_taps, count, first):
    result = jnp.zeros((count, kernel_taps.shape[1]), jnp.float32)
    for offset in range(kernel_taps.shape[0]):
        begin = first + offset
        result = result + kernel_taps[offset] * extended[begin : begin + count]
    return result


def on_device(
    tokens,
    mix_gain,
    query_weight,
    key_weight,
    value_weight,
    conv_value_weight,
    conv_gate_weight,
    query_gain,
    key_gain,
    sink_logit,
    conv_taps,
    conv_gain,
    attn_proj,
    conv_proj,
):
    count = tokens.shape[0]
    packed = jnp.concatenate(
        [query_weight, conv_value_weight, conv_gate_weight, key_weight, value_weight], axis=1
    )
    whole = gather_columns(tokens, "tp")
    weights = gather_line(packed, "sp")
    normed = unit_rows(whole.astype(jnp.float32), mix_gain).astype(jnp.bfloat16)
    projected = jnp.dot(
        normed,
        weights.reshape(-1, packed.shape[1]),
        preferred_element_type=jnp.float32,
    )
    width, channels, kv_width = query_weight.shape[1], conv_taps.shape[1], key_weight.shape[1]
    dim = query_gain.shape[0]
    heads, local_kv = width // dim, kv_width // dim
    at = width + 2 * channels
    conv_value = projected[:, width : width + channels]
    conv_gate = projected[:, width + channels : at]
    keys = unit_rows(projected[:, at : at + kv_width].reshape(count, local_kv, dim), key_gain)
    pairs = jnp.concatenate(
        [
            keys.reshape(count, kv_width).astype(jnp.bfloat16),
            projected[:, at + kv_width :].astype(jnp.bfloat16),
        ],
        axis=1,
    )
    gated = (conv_value * jax.nn.sigmoid(conv_gate)).astype(jnp.bfloat16)
    edge = lambda kv, conv: jnp.concatenate([kv, conv.reshape(-1, 2 * kv_width)], axis=0)
    size = lax.axis_size("sp")
    up = [(i, i + 1) for i in range(size - 1)]
    down = [(j, i) for i, j in up]
    before = lax.ppermute(edge(pairs[count - WINDOW :], gated[count - HALO :]), "sp", up)
    after = lax.ppermute(edge(pairs[:WINDOW], gated[:HALO]), "sp", down)
    kv_rows = jnp.concatenate([before[:WINDOW], pairs, after[:WINDOW]], axis=0)
    conv_rows = jnp.concatenate(
        [
            before[WINDOW:].reshape(HALO, channels),
            gated,
            after[WINDOW:].reshape(HALO, channels),
        ],
        axis=0,
    )
    proj = jnp.concatenate([attn_proj, conv_proj], axis=0)
    proj, before, after = lax.optimization_barrier((proj, before, after))
    proj_pieces = gather_line(proj, "sp")
    offset = lax.axis_index("sp") * count
    attended = attend(
        projected, kv_rows, query_gain, sink_logit, offset, count * size, count, heads, local_kv
    )
    reach = (conv_taps.shape[0] - 1) // 2
    convolved = depthwise(conv_rows, conv_taps, count, HALO - reach)
    tp = lax.axis_size("tp")
    mean = jnp.mean(convolved, axis=1)
    apart = convolved - mean[:, None]
    local = jnp.stack([mean, jnp.sum(apart * apart, axis=1)])
    slot = (jnp.arange(tp) == lax.axis_index("tp"))[:, None, None]
    stats = lax.psum(jnp.where(slot, local[None], 0.0), "tp")
    center = jnp.mean(stats[:, 0], axis=0)
    shift = stats[:, 0] - center
    spread = (jnp.sum(stats[:, 1], axis=0) + channels * jnp.sum(shift * shift, axis=0)) / (
        channels * tp
    )
    centered = convolved - center[:, None]
    featured = jax.nn.silu(
        centered * lax.rsqrt(spread[:, None] + EPSILON) * conv_gain
    ).astype(jnp.bfloat16)
    features = jnp.concatenate([attended, featured], axis=1)
    proj_full = proj_pieces.transpose(1, 0, 2).reshape(proj.shape[0], -1)
    partial = jnp.dot(features, proj_full, preferred_element_type=jnp.float32)
    return scatter_sum(partial, "tp").astype(jnp.bfloat16)


def solution(mesh):
    placed = (
        P("sp", "tp"),
        P(),
        P("sp", "tp"),
        P("sp", "tp"),
        P("sp", "tp"),
        P("sp", "tp"),
        P("sp", "tp"),
        P(),
        P(),
        P("tp"),
        P(None, "tp"),
        P("tp"),
        P("tp", "sp"),
        P("tp", "sp"),
    )
    return jax.shard_map(
        on_device, mesh=mesh, in_specs=placed, out_specs=P(("sp", "tp"), None), check_vma=False
    )
```

```python
import jax
import jax.numpy as jnp
from jax import lax
from jax.experimental import pallas as pl
from jax.experimental.pallas import tpu as pltpu
from jax.sharding import PartitionSpec as P

WINDOW = 128
HALO = 16


EPSILON = 0.1


def unit_rows(values, gain):
    return values * lax.rsqrt(jnp.mean(values * values, axis=-1, keepdims=True) + EPSILON) * gain


def gather_columns(tokens, axis):
    size = lax.axis_size(axis)
    if size != 4:
        return lax.all_gather(tokens, axis, axis=1, tiled=True)
    index = lax.axis_index(axis)
    far = lax.ppermute(tokens, axis, [(i, i ^ 2) for i in range(size)])
    near = [(i, i ^ 1) for i in range(size)]
    own_other = lax.ppermute(tokens, axis, near)
    far_other = lax.ppermute(far, axis, near)
    first = index < 2
    even = index % 2 == 0
    own_pair = (jnp.where(even, tokens, own_other), jnp.where(even, own_other, tokens))
    far_pair = (jnp.where(even, far, far_other), jnp.where(even, far_other, far))
    low = [jnp.where(first, a, b) for a, b in zip(own_pair, far_pair)]
    high = [jnp.where(first, b, a) for a, b in zip(own_pair, far_pair)]
    return jnp.concatenate(low + high, axis=1)


def scatter_sum(partial, axis):
    size = lax.axis_size(axis)
    if size != 4:
        blocks = jnp.concatenate([partial(i) for i in range(size)], axis=0)
        return lax.psum_scatter(blocks, axis, scatter_dimension=0, tiled=True)
    index = lax.axis_index(axis)
    near = [(i, i ^ 1) for i in range(size)]
    far = [(i, i ^ 2) for i in range(size)]
    got_away = lax.ppermute(partial(index ^ 3).astype(jnp.bfloat16), axis, near)
    away = partial(index ^ 2) + got_away.astype(jnp.float32)
    came = lax.ppermute(away.astype(jnp.bfloat16), axis, far)
    got_here = lax.ppermute(partial(index ^ 1).astype(jnp.bfloat16), axis, near)
    here = partial(index) + got_here.astype(jnp.float32)
    return here + came.astype(jnp.float32)


def attend(projected, kv, query_gain, sinks, offset, total, count, heads, local_kv):
    dim = query_gain.shape[0]
    group = heads // local_kv
    scale = dim ** (-0.5)
    span = 3 * WINDOW

    def kernel(place, sink, query, pairs, gain, out):
        start = pl.program_id(0) * WINDOW
        window = pairs[pl.ds(pl.multiple_of(start, WINDOW), span), :]
        row = lax.broadcasted_iota(jnp.int32, (WINDOW, span), 0)
        col = lax.broadcasted_iota(jnp.int32, (WINDOW, span), 1)
        key_pos = place[0] + start - WINDOW + col
        allowed = (
            (col >= row) & (col <= row + 2 * WINDOW) & (key_pos >= 0) & (key_pos < total)
        )
        results = []
        for head in range(heads):
            of = head // group
            keys = window[:, of * dim : (of + 1) * dim]
            values = window[:, (local_kv + of) * dim : (local_kv + of + 1) * dim]
            normed = unit_rows(query[:, head * dim : (head + 1) * dim], gain[...])
            scores = lax.dot_general(
                normed.astype(jnp.bfloat16),
                keys,
                (((1,), (1,)), ((), ())),
                preferred_element_type=jnp.float32,
            )
            weights = jnp.where(allowed, jnp.exp(scores * scale), 0.0)
            denominator = jnp.sum(weights, axis=-1, keepdims=True) + sink[head]
            shares = (weights * (1.0 / denominator)).astype(jnp.bfloat16)
            results.append(jnp.dot(shares, values, preferred_element_type=jnp.float32))
        out[...] = jnp.concatenate(results, axis=1).astype(jnp.bfloat16)

    width = heads * dim
    return pl.pallas_call(
        kernel,
        grid=(count // WINDOW,),
        in_specs=[
            pl.BlockSpec(memory_space=pltpu.SMEM),
            pl.BlockSpec(memory_space=pltpu.SMEM),
            pl.BlockSpec((WINDOW, width), lambda i: (i, 0)),
            pl.BlockSpec(kv.shape, lambda i: (0, 0)),
            pl.BlockSpec((1, dim), lambda i: (0, 0)),
        ],
        out_specs=pl.BlockSpec((WINDOW, width), lambda i: (i, 0)),
        out_shape=jax.ShapeDtypeStruct((count, width), jnp.bfloat16),
        name="attend",
    )(offset.reshape(1), jnp.exp(sinks), projected, kv, query_gain.reshape(1, dim))


def depthwise(extended, kernel_taps, count, first):
    result = jnp.zeros((count, kernel_taps.shape[1]), jnp.float32)
    for offset in range(kernel_taps.shape[0]):
        begin = first + offset
        result = result + kernel_taps[offset] * extended[begin : begin + count]
    return result


def on_device(
    tokens,
    mix_gain,
    query_weight,
    key_weight,
    value_weight,
    conv_value_weight,
    conv_gate_weight,
    query_gain,
    key_gain,
    sink_logit,
    conv_taps,
    conv_gain,
    attn_proj,
    conv_proj,
):
    count = tokens.shape[0]
    packed = jnp.concatenate(
        [query_weight, conv_value_weight, conv_gate_weight, key_weight, value_weight], axis=1
    )
    whole = gather_columns(tokens, "tp")
    weights = lax.all_gather(packed, "sp", axis=0, tiled=True)
    normed = unit_rows(whole.astype(jnp.float32), mix_gain).astype(jnp.bfloat16)
    proj = jnp.concatenate([attn_proj, conv_proj], axis=0)
    proj, weights = lax.optimization_barrier((proj, weights))
    proj_pieces = lax.all_gather(proj, "sp", axis=0)
    projected = jnp.dot(
        normed,
        weights,
        preferred_element_type=jnp.float32,
    )
    width, channels, kv_width = query_weight.shape[1], conv_taps.shape[1], key_weight.shape[1]
    dim = query_gain.shape[0]
    heads, local_kv = width // dim, kv_width // dim
    at = width + 2 * channels
    conv_value = projected[:, width : width + channels]
    conv_gate = projected[:, width + channels : at]
    keys = unit_rows(projected[:, at : at + kv_width].reshape(count, local_kv, dim), key_gain)
    pairs = jnp.concatenate(
        [
            keys.reshape(count, kv_width).astype(jnp.bfloat16),
            projected[:, at + kv_width :].astype(jnp.bfloat16),
        ],
        axis=1,
    )
    gated = (conv_value * jax.nn.sigmoid(conv_gate)).astype(jnp.bfloat16)
    edge = lambda kv, conv: jnp.concatenate([kv, conv.reshape(-1, 2 * kv_width)], axis=0)
    size = lax.axis_size("sp")
    up = [(i, i + 1) for i in range(size - 1)]
    down = [(j, i) for i, j in up]
    before = lax.ppermute(edge(pairs[count - WINDOW :], gated[count - HALO :]), "sp", up)
    after = lax.ppermute(edge(pairs[:WINDOW], gated[:HALO]), "sp", down)
    kv_rows = jnp.concatenate([before[:WINDOW], pairs, after[:WINDOW]], axis=0)
    conv_rows = jnp.concatenate(
        [
            before[WINDOW:].reshape(HALO, channels),
            gated,
            after[WINDOW:].reshape(HALO, channels),
        ],
        axis=0,
    )
    offset = lax.axis_index("sp") * count
    attended = attend(
        projected, kv_rows, query_gain, sink_logit, offset, count * size, count, heads, local_kv
    )
    reach = (conv_taps.shape[0] - 1) // 2
    convolved = depthwise(conv_rows, conv_taps, count, HALO - reach)
    tp = lax.axis_size("tp")
    mean = jnp.mean(convolved, axis=1)
    apart = convolved - mean[:, None]
    local = jnp.stack([mean, jnp.sum(apart * apart, axis=1)])
    parts = [local]
    for k in range(1, tp):
        parts.append(lax.ppermute(local, "tp", [(i, (i + k) % tp) for i in range(tp)]))
    stats = jnp.stack(parts)
    center = jnp.mean(stats[:, 0], axis=0)
    shift = stats[:, 0] - center
    spread = (jnp.sum(stats[:, 1], axis=0) + channels * jnp.sum(shift * shift, axis=0)) / (
        channels * tp
    )
    centered = convolved - center[:, None]
    featured = jax.nn.silu(
        centered * lax.rsqrt(spread[:, None] + EPSILON) * conv_gain
    ).astype(jnp.bfloat16)
    features = jnp.concatenate([attended, featured], axis=1)
    proj_full = proj_pieces.transpose(1, 0, 2).reshape(proj.shape[0], -1)
    rows = count // tp

    def partial(block):
        taken = lax.dynamic_slice_in_dim(features, block * rows, rows, 0)
        return jnp.dot(taken, proj_full, preferred_element_type=jnp.float32)

    return scatter_sum(partial, "tp").astype(jnp.bfloat16)


def solution(mesh):
    placed = (
        P("sp", "tp"),
        P(),
        P("sp", "tp"),
        P("sp", "tp"),
        P("sp", "tp"),
        P("sp", "tp"),
        P("sp", "tp"),
        P(),
        P(),
        P("tp"),
        P(None, "tp"),
        P("tp"),
        P("tp", "sp"),
        P("tp", "sp"),
    )
    return jax.shard_map(
        on_device, mesh=mesh, in_specs=placed, out_specs=P(("sp", "tp"), None), check_vma=False
    )
```

```python
import jax
import jax.numpy as jnp
from jax import lax
from jax.experimental import pallas as pl
from jax.experimental.pallas import tpu as pltpu
from jax.sharding import PartitionSpec as P

WINDOW = 128
HALO = 16


EPSILON = 0.1


def unit_rows(values, gain):
    return values * lax.rsqrt(jnp.mean(values * values, axis=-1, keepdims=True) + EPSILON) * gain


def gather_columns(tokens, axis):
    size = lax.axis_size(axis)
    if size != 4:
        return lax.all_gather(tokens, axis, axis=1, tiled=True)
    index = lax.axis_index(axis)
    far = lax.ppermute(tokens, axis, [(i, i ^ 2) for i in range(size)])
    near = [(i, i ^ 1) for i in range(size)]
    own_other = lax.ppermute(tokens, axis, near)
    far_other = lax.ppermute(far, axis, near)
    first = index < 2
    even = index % 2 == 0
    own_pair = (jnp.where(even, tokens, own_other), jnp.where(even, own_other, tokens))
    far_pair = (jnp.where(even, far, far_other), jnp.where(even, far_other, far))
    low = [jnp.where(first, a, b) for a, b in zip(own_pair, far_pair)]
    high = [jnp.where(first, b, a) for a, b in zip(own_pair, far_pair)]
    return jnp.concatenate(low + high, axis=1)


def scatter_sum(partial, axis):
    size = lax.axis_size(axis)
    if size != 4:
        blocks = jnp.concatenate([partial(i) for i in range(size)], axis=0)
        return lax.psum_scatter(blocks, axis, scatter_dimension=0, tiled=True)
    index = lax.axis_index(axis)
    near = [(i, i ^ 1) for i in range(size)]
    far = [(i, i ^ 2) for i in range(size)]
    got_away = lax.ppermute(partial(index ^ 3).astype(jnp.bfloat16), axis, near)
    away = partial(index ^ 2) + got_away.astype(jnp.float32)
    came = lax.ppermute(away.astype(jnp.bfloat16), axis, far)
    got_here = lax.ppermute(partial(index ^ 1).astype(jnp.bfloat16), axis, near)
    here = partial(index) + got_here.astype(jnp.float32)
    return here + came.astype(jnp.float32)


def attend(projected, kv, query_gain, sinks, offset, total, count, heads, local_kv):
    dim = query_gain.shape[0]
    group = heads // local_kv
    scale = dim ** (-0.5)
    span = 3 * WINDOW

    def kernel(place, sink, query, pairs, gain, out):
        start = pl.program_id(0) * WINDOW
        window = pairs[pl.ds(pl.multiple_of(start, WINDOW), span), :]
        row = lax.broadcasted_iota(jnp.int32, (WINDOW, span), 0)
        col = lax.broadcasted_iota(jnp.int32, (WINDOW, span), 1)
        key_pos = place[0] + start - WINDOW + col
        allowed = (
            (col >= row) & (col <= row + 2 * WINDOW) & (key_pos >= 0) & (key_pos < total)
        )
        results = []
        for head in range(heads):
            of = head // group
            keys = window[:, of * dim : (of + 1) * dim]
            values = window[:, (local_kv + of) * dim : (local_kv + of + 1) * dim]
            normed = unit_rows(query[:, head * dim : (head + 1) * dim], gain[...])
            scores = lax.dot_general(
                normed.astype(jnp.bfloat16),
                keys,
                (((1,), (1,)), ((), ())),
                preferred_element_type=jnp.float32,
            )
            weights = jnp.where(allowed, jnp.exp(scores * scale), 0.0)
            denominator = jnp.sum(weights, axis=-1, keepdims=True) + sink[head]
            shares = (weights * (1.0 / denominator)).astype(jnp.bfloat16)
            results.append(jnp.dot(shares, values, preferred_element_type=jnp.float32))
        out[...] = jnp.concatenate(results, axis=1).astype(jnp.bfloat16)

    width = heads * dim
    return pl.pallas_call(
        kernel,
        grid=(count // WINDOW,),
        in_specs=[
            pl.BlockSpec(memory_space=pltpu.SMEM),
            pl.BlockSpec(memory_space=pltpu.SMEM),
            pl.BlockSpec((WINDOW, width), lambda i: (i, 0)),
            pl.BlockSpec(kv.shape, lambda i: (0, 0)),
            pl.BlockSpec((1, dim), lambda i: (0, 0)),
        ],
        out_specs=pl.BlockSpec((WINDOW, width), lambda i: (i, 0)),
        out_shape=jax.ShapeDtypeStruct((count, width), jnp.bfloat16),
        name="attend",
    )(offset.reshape(1), jnp.exp(sinks), projected, kv, query_gain.reshape(1, dim))


def depthwise(extended, kernel_taps, count, first):
    result = jnp.zeros((count, kernel_taps.shape[1]), jnp.float32)
    for offset in range(kernel_taps.shape[0]):
        begin = first + offset
        result = result + kernel_taps[offset] * extended[begin : begin + count]
    return result


def on_device(
    tokens,
    mix_gain,
    query_weight,
    key_weight,
    value_weight,
    conv_value_weight,
    conv_gate_weight,
    query_gain,
    key_gain,
    sink_logit,
    conv_taps,
    conv_gain,
    attn_proj,
    conv_proj,
):
    count = tokens.shape[0]
    packed = jnp.concatenate(
        [query_weight, conv_value_weight, conv_gate_weight, key_weight, value_weight], axis=1
    )
    whole = gather_columns(tokens, "tp")
    weights = lax.all_gather(packed, "sp", axis=0, tiled=True)
    normed = unit_rows(whole.astype(jnp.float32), mix_gain).astype(jnp.bfloat16)
    proj = jnp.concatenate([attn_proj, conv_proj], axis=0)
    proj, _ = lax.optimization_barrier((proj, whole[:1, :1]))
    proj_pieces = lax.all_gather(proj, "sp", axis=0)
    projected = jnp.dot(
        normed,
        weights,
        preferred_element_type=jnp.float32,
    )
    width, channels, kv_width = query_weight.shape[1], conv_taps.shape[1], key_weight.shape[1]
    dim = query_gain.shape[0]
    heads, local_kv = width // dim, kv_width // dim
    at = width + 2 * channels
    conv_value = projected[:, width : width + channels]
    conv_gate = projected[:, width + channels : at]
    keys = unit_rows(projected[:, at : at + kv_width].reshape(count, local_kv, dim), key_gain)
    pairs = jnp.concatenate(
        [
            keys.reshape(count, kv_width).astype(jnp.bfloat16),
            projected[:, at + kv_width :].astype(jnp.bfloat16),
        ],
        axis=1,
    )
    gated = (conv_value * jax.nn.sigmoid(conv_gate)).astype(jnp.bfloat16)
    edge = lambda kv, conv: jnp.concatenate([kv, conv.reshape(-1, 2 * kv_width)], axis=0)
    size = lax.axis_size("sp")
    up = [(i, i + 1) for i in range(size - 1)]
    down = [(j, i) for i, j in up]
    before = lax.ppermute(edge(pairs[count - WINDOW :], gated[count - HALO :]), "sp", up)
    after = lax.ppermute(edge(pairs[:WINDOW], gated[:HALO]), "sp", down)
    kv_rows = jnp.concatenate([before[:WINDOW], pairs, after[:WINDOW]], axis=0)
    conv_rows = jnp.concatenate(
        [
            before[WINDOW:].reshape(HALO, channels),
            gated,
            after[WINDOW:].reshape(HALO, channels),
        ],
        axis=0,
    )
    offset = lax.axis_index("sp") * count
    attended = attend(
        projected, kv_rows, query_gain, sink_logit, offset, count * size, count, heads, local_kv
    )
    reach = (conv_taps.shape[0] - 1) // 2
    convolved = depthwise(conv_rows, conv_taps, count, HALO - reach)
    tp = lax.axis_size("tp")
    mean = jnp.mean(convolved, axis=1)
    apart = convolved - mean[:, None]
    local = jnp.stack([mean, jnp.sum(apart * apart, axis=1)])
    parts = [local]
    for k in range(1, tp):
        parts.append(lax.ppermute(local, "tp", [(i, (i + k) % tp) for i in range(tp)]))
    stats = jnp.stack(parts)
    center = jnp.mean(stats[:, 0], axis=0)
    shift = stats[:, 0] - center
    spread = (jnp.sum(stats[:, 1], axis=0) + channels * jnp.sum(shift * shift, axis=0)) / (
        channels * tp
    )
    centered = convolved - center[:, None]
    featured = jax.nn.silu(
        centered * lax.rsqrt(spread[:, None] + EPSILON) * conv_gain
    ).astype(jnp.bfloat16)
    features = jnp.concatenate([attended, featured], axis=1)
    proj_full = proj_pieces.transpose(1, 0, 2).reshape(proj.shape[0], -1)
    rows = count // tp

    def partial(block):
        taken = lax.dynamic_slice_in_dim(features, block * rows, rows, 0)
        return jnp.dot(taken, proj_full, preferred_element_type=jnp.float32)

    return scatter_sum(partial, "tp").astype(jnp.bfloat16)


def solution(mesh):
    placed = (
        P("sp", "tp"),
        P(),
        P("sp", "tp"),
        P("sp", "tp"),
        P("sp", "tp"),
        P("sp", "tp"),
        P("sp", "tp"),
        P(),
        P(),
        P("tp"),
        P(None, "tp"),
        P("tp"),
        P("tp", "sp"),
        P("tp", "sp"),
    )
    return jax.shard_map(
        on_device, mesh=mesh, in_specs=placed, out_specs=P(("sp", "tp"), None), check_vma=False
    )
```
